32 devices in a mesh: sp: 8 (over z, y), tp: 4 (over x, core).
Axes of the slice: x: 2, y: 2, z: 4, core: 2. Of those that a mesh axis runs over, the one named last changes fastest.
Arguments:
- arriving_hidden_state: bfloat16 [8192, 2048], P(('sp', 'tp')), may hold values from -6 to 6
- former_request_vectors: bfloat16 [8192, 1024], P('sp', 'tp'), may hold values from -6 to 6
- former_match_vectors: bfloat16 [8192, 1024], P('sp', 'tp'), may hold values from -6 to 6
- latter_request_vectors: bfloat16 [8192, 512], P('sp', 'tp'), may hold values from -6 to 6
- latter_match_vectors: bfloat16 [8192, 512], P('sp', 'tp'), may hold values from -6 to 6
- stored_vectors_both: bfloat16 [8192, 2, 1024], P('sp', None, 'tp'), may hold values from -6 to 6
- closing_valve_operands: bfloat16 [8192, 2, 1024], P('sp', None, 'tp'), may hold values from -6 to 6
- update_level_before_squash: bfloat16 [2, 8, 8192], P(None, 'tp', 'sp'), may hold values from -4 to -3
- fading_data_input: float32 [2, 8, 8192], P(None, 'tp', 'sp'), may hold values from -5.5 to 5.5
- sparse_fading_boost: float32 [2, 8, 8192], P(None, 'tp', 'sp'), may hold values from -2 to 0, as said below
- unitwise_fading_loglevel: float32 [2, 8], P(None, 'tp'), as said below
- fading_constant_term: float32 [2, 8], P(None, 'tp'), may hold values from -1 to 1
- unitwise_normalizer_coef: float32 [128], replicated, may hold values from 0.1 to 1.9
- emission_map_weights: bfloat16 [2048, 2048], replicated, may hold values from -0.125 to 0.125
- channel_normalizer_coef: float32 [2048], replicated, may hold values from 0.1 to 1.9
- switching_channel_map: bfloat16 [2048, 6144], P('sp', 'tp'), may hold values from -0.125 to 0.125
- broadening_channel_map: bfloat16 [2048, 6144], P('sp', 'tp'), may hold values from -0.125 to 0.125
- timewise_convolve_tapvalues: bfloat16 [3, 2, 6144], P(None, None, 'tp'), may hold values from -3.5 to 3.5
- narrowing_map_weights_in: bfloat16 [2048, 6144], P('sp', 'tp'), may hold values from -0.078125 to 0.078125
Outputs:
- mixed: bfloat16 [8192, 2048], P(('sp', 'tp'))
The draws below stay inside these ranges and needn't reach their ends.
Inputs may be any that keep to these rules, and one draw needn't show every extreme that they name: `unitwise_fading_loglevel`: each entry is the logarithm of a per-position rate between 0.2 / 8192 and 2 / 64. `sparse_fading_boost`: zero except at three or fewer positions of the sequence.
All inputs are finite; a program needn't handle non-finite values.
Results may differ from the reference program's by a relative error of at most 0.015.
Values may be sent and summed in bfloat16 or wider, within the bound.
No kernel may reach another device: no remote copies, remote signals or barrier semaphores. Data moves between devices by JAX's collectives and lax.ppermute only.
A program may use at most 128 MiB of HBM per device.

```python
import jax
import jax.numpy as jnp
from jax import lax

MODEL_WIDTH = 2048
ATTN_UNITS = 8
DK_ONE = 128
DK_TWO = 64
VALUE_DIM = 128
FF = 6144
SPAN = 64
TAPS = 3
TOK_DEV = 1024
STEP_TOTAL = 8192
VW = 2048
N_TP = 4


def drawn_keys(key, column_count):
    direction_key, jitter_key = jax.random.split(key)
    directions = jax.random.normal(direction_key, (STEP_TOTAL // SPAN, column_count), jnp.float32)
    repeated = jnp.repeat(directions, SPAN, axis=0)
    jitter = jax.random.normal(jitter_key, (STEP_TOTAL, column_count), jnp.float32)
    jitter_scale = 0.2
    return jnp.clip(repeated + jitter_scale * jitter, -6.0, 6.0).astype(jnp.bfloat16)


def draw_former_match_vectors(key, part):
    return drawn_keys(jax.random.fold_in(key, 71), ATTN_UNITS * DK_ONE)


def draw_latter_match_vectors(key, part):
    return drawn_keys(jax.random.fold_in(key, 79), ATTN_UNITS * DK_TWO)


def draw_update_level_before_squash(key, part):
    drawn = jax.random.uniform(jax.random.fold_in(key, 53), (2, ATTN_UNITS, STEP_TOTAL), jnp.float32, -4.0, -3.0)
    return drawn.astype(jnp.bfloat16)


def draw_fading_data_input(key, part):
    noise_key, shift_key = jax.random.split(jax.random.fold_in(key, 11))
    noise_draw = jax.random.truncated_normal(noise_key, -4.0, 4.0, (2, ATTN_UNITS, STEP_TOTAL), jnp.float32)
    offsets = jax.random.uniform(shift_key, (2, ATTN_UNITS, STEP_TOTAL // TOK_DEV), jnp.float32, -1.5, 1.5)
    offset_rows = jnp.repeat(offsets, TOK_DEV, axis=2)
    return noise_draw + offset_rows


def draw_sparse_fading_boost(key, part):
    position_random_key, size_key = jax.random.split(jax.random.fold_in(key, 23))
    spike_positions = jax.random.randint(position_random_key, (3,), 0, STEP_TOTAL)
    kept_share = jax.random.uniform(size_key, (2, ATTN_UNITS, 3), jnp.float32, 0.55, 0.8)
    position_hits = (jnp.arange(STEP_TOTAL)[None, :] == spike_positions[:, None]).astype(jnp.float32)
    return jnp.einsum('ghb,bs->ghs', jnp.log(kept_share), position_hits)


def draw_unitwise_fading_loglevel(key, part):
    pick_key, fast_key, slow_key = jax.random.split(jax.random.fold_in(key, 37), 3)
    fast_share = 0.5
    fast_mask = jax.random.uniform(pick_key, (2, ATTN_UNITS), jnp.float32) < fast_share
    fast_rate = jax.random.uniform(fast_key, (2, ATTN_UNITS), jnp.float32, 1.0, 2.0) / SPAN
    slow_rate = jax.random.uniform(slow_key, (2, ATTN_UNITS), jnp.float32, 0.2, 0.4) / STEP_TOTAL
    return jnp.log(jnp.where(fast_mask, fast_rate, slow_rate))


def level_of(key, dims, cuts, smallest, high):
    loudness, own = 1.0, jax.random.fold_in(key, 6)
    for axis_at, shards_of in cuts:
        heights = jnp.exp(jax.random.uniform(jax.random.fold_in(own, axis_at), (shards_of,), jnp.float32, smallest / len(cuts), high / len(cuts)))
        loudness = loudness * jnp.repeat(heights, dims[axis_at] // shards_of).reshape([-1 if axis == axis_at else 1 for axis in range(len(dims))])
    return loudness


def gaussian(rng, shape, scale, most, shards=(), kind=jnp.bfloat16):
    entries = jax.random.normal(rng, shape, jnp.float32) * scale
    if len(shards) > 0:
        entries = level_of(rng, shape, shards, -0.22, 0.18) * entries
    return jnp.clip(entries, min=-most, max=most).astype(kind)


def setup_inputs(seed: int = 0) -> dict:
    streams_of = jax.random.split(jax.random.key(seed), 20)
    return {
        "arriving_hidden_state": gaussian(streams_of[0], (STEP_TOTAL, MODEL_WIDTH), 1.0, 6.0, ((0, 32),)),
        "former_request_vectors": gaussian(streams_of[1], (STEP_TOTAL, ATTN_UNITS * DK_ONE), 1.0, 6.0, ((0, 8), (1, 4))),
        "former_match_vectors": draw_former_match_vectors(jax.random.fold_in(streams_of[19], 71), 0),
        "latter_request_vectors": gaussian(streams_of[3], (STEP_TOTAL, ATTN_UNITS * DK_TWO), 1.0, 6.0, ((0, 8), (1, 4))),
        "latter_match_vectors": draw_latter_match_vectors(jax.random.fold_in(streams_of[19], 71), 0),
        "stored_vectors_both": gaussian(streams_of[5], (STEP_TOTAL, 2, ATTN_UNITS * VALUE_DIM), 1.0, 6.0, ((0, 8), (2, 4))),
        "closing_valve_operands": gaussian(streams_of[6], (STEP_TOTAL, 2, ATTN_UNITS * VALUE_DIM), 1.0, 6.0, ((0, 8), (2, 4))),
        "update_level_before_squash": draw_update_level_before_squash(jax.random.fold_in(streams_of[19], 71), 0),
        "fading_data_input": draw_fading_data_input(jax.random.fold_in(streams_of[19], 71), 0),
        "sparse_fading_boost": draw_sparse_fading_boost(jax.random.fold_in(streams_of[19], 71), 0),
        "unitwise_fading_loglevel": draw_unitwise_fading_loglevel(jax.random.fold_in(streams_of[19], 71), 0),
        "fading_constant_term": jnp.clip(jax.random.uniform(streams_of[11], (2, ATTN_UNITS), jnp.float32, -1.0, 1.0) * level_of(streams_of[11], (2, ATTN_UNITS), ((1, 4),), -0.4, 0.0), -1.0, 1.0),
        "unitwise_normalizer_coef": jnp.clip(1.0 + 0.18 * jax.random.normal(streams_of[12], (VALUE_DIM,), jnp.float32), 0.1, 1.9),
        "emission_map_weights": gaussian(streams_of[13], (VW, MODEL_WIDTH), VW ** -0.5, 0.125),
        "channel_normalizer_coef": jnp.clip(1.0 + 0.18 * jax.random.normal(streams_of[14], (MODEL_WIDTH,), jnp.float32), 0.1, 1.9),
        "switching_channel_map": gaussian(streams_of[15], (MODEL_WIDTH, FF), MODEL_WIDTH ** -0.5, 0.125, ((0, 8), (1, 4))),
        "broadening_channel_map": gaussian(streams_of[16], (MODEL_WIDTH, FF), MODEL_WIDTH ** -0.5, 0.125, ((0, 8), (1, 4))),
        "timewise_convolve_tapvalues": gaussian(streams_of[17], (TAPS, 2, FF), TAPS ** -0.5, 3.5, ((2, 4),)),
        "narrowing_map_weights_in": gaussian(streams_of[18], (MODEL_WIDTH, FF), FF ** -0.5, 0.078125, ((0, 8), (1, 4))),
    }


EPSILON = 1e-06
PRECISE = lax.Precision.HIGHEST

def unit_rows(matrix):
    return matrix * lax.rsqrt(lax.optimization_barrier(jnp.sum(matrix * matrix, axis=-1, keepdims=True)) + EPSILON)

def heads_first(matrix, head_count):
    row_count = matrix.shape[0]
    return matrix.reshape(row_count, head_count, -1).astype(jnp.float32).transpose(1, 0, 2)

def block_terms(queries, key_rows, value_rows, beta_rate, gate_logarithms):
    head_count, length, key_size = queries.shape
    num_blocks = length // SPAN
    queries = queries.reshape(head_count, num_blocks, SPAN, -1)
    key_rows = key_rows.reshape(head_count, num_blocks, SPAN, -1)
    value_rows = value_rows.reshape(head_count, num_blocks, SPAN, -1)
    beta_rate = beta_rate.reshape(head_count, num_blocks, SPAN)
    cum_gates = jnp.cumsum(gate_logarithms.reshape(head_count, num_blocks, SPAN), axis=-1)
    row_pos = lax.broadcasted_iota(jnp.int32, (SPAN, SPAN), 0)
    col_pos = lax.broadcasted_iota(jnp.int32, (SPAN, SPAN), 1)
    causal = row_pos >= col_pos
    strict = row_pos > col_pos
    decay = jnp.exp(jnp.where(causal, cum_gates[..., :, None] - cum_gates[..., None, :], -jnp.inf))
    key_beta = key_rows * beta_rate[..., None]
    lower = jnp.where(strict, jnp.einsum('hncd,hnsd->hncs', key_beta, key_rows, precision=PRECISE) * decay, 0.0)
    right_side = jnp.concatenate([value_rows * beta_rate[..., None], key_beta * jnp.exp(cum_gates)[..., None]], axis=-1)
    unit_mat = jnp.eye(SPAN, dtype=lower.dtype)
    solved = lax.linalg.triangular_solve(lower + unit_mat, right_side, left_side=True, lower=True, unit_diagonal=True)
    value_size = value_rows.shape[-1]
    u_values = solved[..., :value_size]
    w_keys = solved[..., value_size:]
    intra = jnp.einsum('hncd,hnsd->hncs', queries, key_rows, precision=PRECISE) * decay
    key_decayed = key_rows * jnp.exp(cum_gates[..., -1:] - cum_gates)[..., None]
    return (queries, u_values, w_keys, intra, key_decayed, cum_gates)

def run_blocks(increment_list, initial_memory):

    def advance(state_mat, inputs):
        query_blk, u_blk, w_blk, intra_blk, kdec_blk, cum_blk = inputs
        fresh = u_blk - jnp.einsum('hcd,hde->hce', w_blk, state_mat, precision=PRECISE)
        output = jnp.einsum('hcd,hde->hce', query_blk * jnp.exp(cum_blk)[..., None], state_mat, precision=PRECISE)
        output = output + jnp.einsum('hcs,hse->hce', intra_blk, fresh, precision=PRECISE)
        state_mat = state_mat * jnp.exp(cum_blk[:, -1])[:, None, None]
        state_mat = state_mat + jnp.einsum('hcd,hce->hde', kdec_blk, fresh, precision=PRECISE)
        return (state_mat, output)
    moved = tuple((jnp.moveaxis(member, 1, 0) for member in increment_list))
    _, outputs = lax.scan(advance, initial_memory, moved)
    head_count = outputs.shape[1]
    return jnp.moveaxis(outputs, 0, 1).reshape(head_count, -1, outputs.shape[-1])

def team_parts(asker_weights, lookup_weights, value_matrix, correction_draw, decay_draw, spike_draw, decay_logarithm, bias_vector):
    head_count = decay_logarithm.shape[0]
    queries = heads_first(asker_weights, head_count)
    key_size = queries.shape[-1]
    queries = unit_rows(queries) * key_size ** (-0.5)
    key_rows = unit_rows(heads_first(lookup_weights, head_count))
    value_rows = heads_first(value_matrix, head_count)
    beta_rate = jax.nn.sigmoid(correction_draw.astype(jnp.float32))
    gate_logarithms = -jnp.exp(decay_logarithm)[:, None] * jax.nn.softplus(decay_draw + bias_vector[:, None]) + spike_draw
    return block_terms(queries, key_rows, value_rows, beta_rate, gate_logarithms)

def completed_attn_units(increment_list, initial_memory, gate_cols, unitwise_normalizer_coef):
    outputs = run_blocks(increment_list, initial_memory)
    head_count = outputs.shape[0]
    gates_in = heads_first(gate_cols, head_count)
    scaled = outputs * lax.rsqrt(lax.optimization_barrier(jnp.mean(outputs * outputs, axis=-1, keepdims=True)) + EPSILON) * unitwise_normalizer_coef
    scaled = scaled * jax.nn.silu(gates_in)
    return scaled.transpose(1, 0, 2).reshape(outputs.shape[1], -1).astype(jnp.bfloat16)

def causal_taps(low_rows, taps_col):
    padded = jnp.concatenate([jnp.zeros((TAPS - 1, low_rows.shape[1]), low_rows.dtype), low_rows], axis=0)
    length = low_rows.shape[0]
    total = taps_col[0] * padded[0:length]
    for tap_index in range(1, TAPS):
        total = total + taps_col[tap_index] * padded[tap_index:tap_index + length]
    return total

def reference(arriving_hidden_state, former_request_vectors, former_match_vectors, latter_request_vectors, latter_match_vectors, stored_vectors_both, closing_valve_operands, update_level_before_squash, fading_data_input, sparse_fading_boost, unitwise_fading_loglevel, fading_constant_term, unitwise_normalizer_coef, emission_map_weights, channel_normalizer_coef, switching_channel_map, broadening_channel_map, timewise_convolve_tapvalues, narrowing_map_weights_in):
    combined_attn_units = []
    pairs = ((former_request_vectors, former_match_vectors), (latter_request_vectors, latter_match_vectors))
    for cohort_ordinal in range(2):
        asker_weights, lookup_weights = pairs[cohort_ordinal]
        increment_list = team_parts(asker_weights, lookup_weights, stored_vectors_both[:, cohort_ordinal], update_level_before_squash[cohort_ordinal], fading_data_input[cohort_ordinal], sparse_fading_boost[cohort_ordinal], unitwise_fading_loglevel[cohort_ordinal], fading_constant_term[cohort_ordinal])
        key_size = increment_list[0].shape[-1]
        head_count = unitwise_fading_loglevel.shape[1]
        initial_memory = jnp.zeros((head_count, key_size, stored_vectors_both.shape[-1] // head_count), jnp.float32)
        combined_attn_units.append(completed_attn_units(increment_list, initial_memory, closing_valve_operands[:, cohort_ordinal], unitwise_normalizer_coef))
    linear_attend = jnp.stack(combined_attn_units, axis=1)
    token_slices = linear_attend.shape[0]
    skip_stream = arriving_hidden_state.astype(jnp.float32) + jnp.dot(linear_attend.reshape(token_slices, -1).astype(jnp.float32), emission_map_weights.astype(jnp.float32), preferred_element_type=jnp.float32)
    normed = (skip_stream * lax.rsqrt(lax.optimization_barrier(jnp.mean(skip_stream * skip_stream, axis=-1, keepdims=True)) + EPSILON) * channel_normalizer_coef).astype(jnp.bfloat16)
    gate_low = jnp.dot(normed.astype(jnp.float32), switching_channel_map.astype(jnp.float32), preferred_element_type=jnp.float32).astype(jnp.bfloat16)
    up_low = jnp.dot(normed.astype(jnp.float32), broadening_channel_map.astype(jnp.float32), preferred_element_type=jnp.float32).astype(jnp.bfloat16)
    taps = timewise_convolve_tapvalues.astype(jnp.float32)
    gate_conv = causal_taps(gate_low, taps[:, 0])
    up_conv = causal_taps(up_low, taps[:, 1])
    hidden = (jax.nn.silu(gate_conv) * up_conv).astype(jnp.bfloat16)
    shard_width = hidden.shape[1] // N_TP
    down_sum = jnp.zeros(skip_stream.shape, jnp.float32)
    for shard_index in range(N_TP):
        lower_col = shard_index * shard_width
        partial_value = lax.dot_general(hidden[:, lower_col:lower_col + shard_width].astype(jnp.float32), narrowing_map_weights_in[:, lower_col:lower_col + shard_width].astype(jnp.float32), (((1,), (1,)), ((), ())), preferred_element_type=jnp.float32)
        down_sum = down_sum + lax.optimization_barrier(partial_value.astype(jnp.bfloat16)).astype(jnp.float32)
    return (skip_stream + down_sum).astype(jnp.bfloat16)
```

```python
import functools

import jax
import jax.numpy as jnp
from jax import lax
from jax.experimental import pallas as pl
from jax.experimental.pallas import tpu as pltpu
from jax.sharding import PartitionSpec as P

TAPS = 3
EPSILON = 1e-06
PRECISE = lax.Precision.HIGHEST
CHUNK = 128
HEADER = 16
F32 = jnp.float32
BF16 = jnp.bfloat16


def mm(a, b, dims=((1,), (0,))):
    return lax.dot_general(a, b, (dims, ((), ())), preferred_element_type=F32)


def exact(a, b, dims=((1,), (0,))):
    return lax.dot_general(a, b, (dims, ((), ())), precision=PRECISE, preferred_element_type=F32)


def kernel_params(mebibytes=56, dims=None):
    return pltpu.CompilerParams(vmem_limit_bytes=mebibytes << 20, dimension_semantics=dims)


def chunk_kernel(head_sizes, value_size, step_chunks, *refs):
    (update, data, spike, level, bias, *rest) = refs
    groups = len(head_sizes)
    queries = rest[:groups]
    keys = rest[groups : 2 * groups]
    values, out_local, out_reach, state_out, state = rest[2 * groups :]
    step = pl.program_id(0)

    @pl.when(step == 0)
    def _():
        top = 0
        for key_size, count in head_sizes:
            for _h in range(count):
                rows = lax.broadcasted_iota(jnp.int32, (key_size, 2 * value_size), 0)
                cols = lax.broadcasted_iota(jnp.int32, (key_size, 2 * value_size), 1)
                state[pl.ds(top, key_size), :] = (cols == rows + value_size).astype(F32)
                top += key_size

    size = CHUNK
    row = lax.broadcasted_iota(jnp.int32, (size, size), 0)
    col = lax.broadcasted_iota(jnp.int32, (size, size), 1)
    causal = row >= col
    strict = row > col
    triangle = causal.astype(F32)
    unit = (row == col).astype(F32)
    beta_all = jax.nn.sigmoid(update[...].astype(F32))
    shifted = data[...] + bias[...]
    softplus = jnp.maximum(shifted, 0.0) + jnp.log(1.0 + jnp.exp(-jnp.abs(shifted)))
    gates_all = -jnp.exp(level[...]) * softplus + spike[...]

    for sub in range(step_chunks):
        lo = sub * size
        beta_row_all = beta_all[:, lo : lo + size]
        gates = gates_all[:, lo : lo + size]
        cum_row_all = exact(gates, triangle, ((1,), (1,)))
        cum_col_all = exact(triangle, gates, ((1,), (1,)))
        beta_col_all = exact(unit, beta_row_all, ((1,), (1,)))
        top = 0
        number = 0
        for g, (key_size, count) in enumerate(head_sizes):
            reach_parts = []
            for h in range(count):
                kb = keys[g][pl.ds(lo, size), h * key_size : (h + 1) * key_size]
                qb = queries[g][pl.ds(lo, size), h * key_size : (h + 1) * key_size]
                vcol = number * value_size
                vb = values[pl.ds(lo, size), vcol : vcol + value_size]
                kf = kb.astype(F32)
                qf = qb.astype(F32)
                ksq = kf * kf
                rk = lax.rsqrt(jnp.sum(ksq, axis=1, keepdims=True) + EPSILON)
                rq = lax.rsqrt(jnp.sum(qf * qf, axis=1, keepdims=True) + EPSILON) * key_size**-0.5
                ones = jnp.ones((8, key_size), F32)
                rk_row = lax.rsqrt(exact(ones, ksq, ((1,), (1,)))[0:1] + EPSILON)
                cum_row = cum_row_all[number : number + 1]
                beta_row = beta_row_all[number : number + 1]
                cum = cum_col_all[:, number : number + 1]
                beta = beta_col_all[:, number : number + 1]
                last = cum_row[:, size - 1 : size]
                decay = jnp.exp(jnp.where(causal, cum - cum_row, -1e30)) * rk_row
                lower = jnp.where(strict, mm(kb, kb, ((1,), (1,))) * decay * (beta * rk), 0.0)
                intra = mm(qb, kb, ((1,), (1,))) * decay * rq
                width = 1
                inverse = unit
                while width < size:
                    span = 2 * width
                    off = (row // span == col // span) & (row // width != col // width)
                    part = jnp.where(off, lower, 0.0)
                    if width == 1:
                        inverse = unit - part
                    else:
                        xb = inverse.astype(BF16)
                        inverse = inverse - mm(xb, mm(part.astype(BF16), xb).astype(BF16))
                    width = span
                u_values = mm((inverse * beta_row).astype(BF16), vb)
                w_keys = mm((inverse * (beta_row * rk_row * jnp.exp(cum_row))).astype(BF16), kb)
                old = state[pl.ds(top, key_size), :]
                old_b = old.astype(BF16)
                pulled = mm(w_keys.astype(BF16), old_b)
                fresh = jnp.concatenate(
                    [u_values - pulled[:, :value_size], -pulled[:, value_size:]], axis=1
                )
                result = mm(qb, old_b) * (rq * jnp.exp(cum)) + mm(intra.astype(BF16), fresh.astype(BF16))
                scaled = (fresh * (rk * jnp.exp(last - cum))).astype(BF16)
                state[pl.ds(top, key_size), :] = old * jnp.exp(last) + mm(kb, scaled, ((0,), (0,)))
                out_local[pl.ds(lo, size), vcol : vcol + value_size] = result[:, :value_size]
                reach_parts.append(result[:, value_size : value_size + key_size])
                top += key_size
                number += 1
            reach = jnp.concatenate(reach_parts, axis=1).astype(BF16)
            left = sum(k * c for k, c in head_sizes[:g])
            out_reach[pl.ds(lo, size), left : left + reach.shape[1]] = reach

    @pl.when(step == pl.num_programs(0) - 1)
    def _():
        state_out[...] = state[...].astype(BF16)


def attention_pass(head_sizes, queries, keys, values, update, data, spike, level, bias):
    rows = values.shape[0]
    heads = sum(c for _, c in head_sizes)
    value_size = values.shape[1] // heads
    step_chunks = 2
    tile = CHUNK * step_chunks
    key_cols = sum(k * c for k, c in head_sizes)
    by_rows = lambda a: pl.BlockSpec((tile, a.shape[1]), lambda i: (i, 0))
    by_cols = lambda a: pl.BlockSpec((a.shape[0], tile), lambda i: (0, i))
    whole = lambda a: pl.BlockSpec(a.shape, lambda i: (0, 0))
    return pl.pallas_call(
        functools.partial(chunk_kernel, head_sizes, value_size, step_chunks),
        grid=(rows // tile,),
        in_specs=[by_cols(update), by_cols(data), by_cols(spike), whole(level), whole(bias)]
        + [by_rows(a) for a in (*queries, *keys, values)],
        out_specs=[
            pl.BlockSpec((tile, heads * value_size), lambda i: (i, 0)),
            pl.BlockSpec((tile, key_cols), lambda i: (i, 0)),
            pl.BlockSpec((key_cols, 2 * value_size), lambda i: (0, 0)),
        ],
        out_shape=[
            jax.ShapeDtypeStruct((rows, heads * value_size), F32),
            jax.ShapeDtypeStruct((rows, key_cols), BF16),
            jax.ShapeDtypeStruct((key_cols, 2 * value_size), BF16),
        ],
        scratch_shapes=[pltpu.VMEM((key_cols, 2 * value_size), F32)],
        compiler_params=kernel_params(dims=("arbitrary",)),
        name="attention_pass",
    )(update, data, spike, level, bias, *queries, *keys, values)


def joined(head_sizes, value_size, later, earlier, columns):
    parts = []
    top = 0
    for key_size, count in head_sizes:
        for _h in range(count):
            moves = later[top : top + key_size, value_size : value_size + key_size]
            new = mm(moves, earlier[top : top + key_size, :columns])
            adds = later[top : top + key_size, :value_size].astype(F32)
            if columns > value_size:
                new = jnp.concatenate([new[:, :value_size] + adds, new[:, value_size:]], axis=1)
            else:
                new = new + adds
            parts.append(new)
            top += key_size
    return jnp.concatenate(parts, axis=0)


def pair_kernel(head_sizes, value_size, odd, own, other, out):
    is_odd = odd[0] == 1
    mine = own[...]
    theirs = other[...]
    later = jnp.where(is_odd, mine, theirs)
    earlier = jnp.where(is_odd, theirs, mine)
    out[...] = joined(head_sizes, value_size, later, earlier, mine.shape[1]).astype(BF16)


def chain_kernel(head_sizes, value_size, later, earlier, out):
    out[...] = joined(head_sizes, value_size, later[...], earlier[...], out.shape[1]).astype(BF16)


def join_pair(head_sizes, value_size, odd, own, other):
    return pl.pallas_call(
        functools.partial(pair_kernel, head_sizes, value_size),
        in_specs=[pl.BlockSpec(memory_space=pltpu.SMEM), pl.BlockSpec(), pl.BlockSpec()],
        out_shape=jax.ShapeDtypeStruct(own.shape, BF16),
        name="join_pair",
    )(odd, own, other)


def join_chain(head_sizes, value_size, later, earlier):
    return pl.pallas_call(
        functools.partial(chain_kernel, head_sizes, value_size),
        out_shape=jax.ShapeDtypeStruct(earlier.shape, BF16),
        name="join_chain",
    )(later, earlier)


def shifted(value, axis, steps):
    count = lax.axis_size(axis)
    return lax.ppermute(value, axis, [(i, i + steps) for i in range(count - steps)])


def swapped(value, axis, mask):
    count = lax.axis_size(axis)
    return lax.ppermute(value, axis, [(i, i ^ mask) for i in range(count)])


def state_before(head_sizes, value_size, summary):
    count = lax.axis_size("sp")
    odd = jnp.full((1,), lax.axis_index("sp") % 2, jnp.int32)
    partner = swapped(summary, "sp", 1)
    pair = join_pair(head_sizes, value_size, odd, summary, partner)
    before = shifted(pair, "sp", 2)
    covered, pairs = 1, count // 2
    while covered < pairs - 1:
        window = join_chain(head_sizes, value_size, pair, before)
        reach = covered + 1
        finishing = covered + reach >= pairs - 1
        sent = window[:, :value_size] if finishing else window
        arrived = shifted(sent, "sp", 2 * reach)
        before = join_chain(head_sizes, value_size, before, arrived)
        covered += reach
    return odd, before[:, :value_size], partner


def finish_kernel(head_sizes, value_size, odd, before, partner, local, reach, gates, coef, out, initial):
    @pl.when(pl.program_id(0) == 0)
    def _():
        entering = before[...]
        through = joined(head_sizes, value_size, partner[...], entering, value_size)
        initial[...] = jnp.where(odd[0] == 1, through, entering.astype(F32)).astype(BF16)

    top = 0
    number = 0
    for key_size, count in head_sizes:
        for _h in range(count):
            cols = slice(number * value_size, (number + 1) * value_size)
            full = local[:, cols] + mm(
                reach[:, top : top + key_size], initial[pl.ds(top, key_size), :]
            )
            gate = gates[:, cols].astype(F32)
            size = lax.rsqrt(jnp.mean(full * full, axis=1, keepdims=True) + EPSILON)
            out[:, cols] = (full * size * coef[...] * (gate * jax.nn.sigmoid(gate))).astype(BF16)
            top += key_size
            number += 1


def finish_heads(head_sizes, value_size, odd, before, partner, local, reach, gates, coef):
    rows = local.shape[0]
    tile = min(rows, 256)
    by_rows = lambda a: pl.BlockSpec((tile, a.shape[1]), lambda i: (i, 0))
    whole = lambda a: pl.BlockSpec(a.shape, lambda i: (0, 0))
    return pl.pallas_call(
        functools.partial(finish_kernel, head_sizes, value_size),
        grid=(rows // tile,),
        in_specs=[
            pl.BlockSpec(memory_space=pltpu.SMEM),
            whole(before),
            whole(partner),
            by_rows(local),
            by_rows(reach),
            by_rows(gates),
            whole(coef),
        ],
        out_specs=by_rows(local),
        out_shape=jax.ShapeDtypeStruct(local.shape, BF16),
        scratch_shapes=[pltpu.VMEM(before.shape, BF16)],
        compiler_params=kernel_params(dims=("arbitrary",)),
        name="finish_heads",
    )(odd, before, partner, local, reach, gates, coef)


def emission_kernel(arrived, weights, stream, coef, resid, normed, total):
    step = pl.program_id(0)
    part = mm(arrived[0], weights[...])

    @pl.when(step == 0)
    def _():
        total[...] = stream[...].astype(F32) + part

    @pl.when(step > 0)
    def _():
        total[...] += part

    @pl.when(step == pl.num_programs(0) - 1)
    def _():
        full = total[...]
        resid[...] = full
        size = lax.rsqrt(jnp.mean(full * full, axis=1, keepdims=True) + EPSILON)
        normed[...] = (full * size * coef[...]).astype(BF16)


def emission(arrived, weights, stream, coef, groups):
    senders, rows, cols = arrived.shape
    part = cols // groups
    width = stream.shape[1]
    whole = pl.BlockSpec((rows, width), lambda i: (0, 0))
    return pl.pallas_call(
        emission_kernel,
        grid=(senders * groups,),
        in_specs=[
            pl.BlockSpec((1, rows, part), lambda i: (i // groups, 0, i % groups)),
            pl.BlockSpec((part, width), lambda i: ((i % groups) * senders + i // groups, 0)),
            whole,
            pl.BlockSpec((1, width), lambda i: (0, 0)),
        ],
        out_specs=[whole, whole],
        out_shape=[
            jax.ShapeDtypeStruct((rows, width), F32),
            jax.ShapeDtypeStruct((rows, width), BF16),
        ],
        scratch_shapes=[pltpu.VMEM((rows, width), F32)],
        compiler_params=kernel_params(dims=("arbitrary",)),
        name="emission",
    )(arrived, weights, stream, coef)


def convolved(low, taps, rows):
    total = None
    for j in range(TAPS):
        start = HEADER - (TAPS - 1) + j
        term = taps[j : j + 1, :] * low[start : start + rows, :]
        total = term if total is None else total + term
    return total


def hidden_kernel(slabs, features, edges, gate_w, up_w, taps, out):
    taken = jnp.concatenate(
        [piece for s in range(slabs) for piece in (edges[s], features[s])], axis=0
    )
    gate_low = mm(taken, gate_w[...]).astype(BF16).astype(F32)
    up_low = mm(taken, up_w[...]).astype(BF16).astype(F32)
    rows = features.shape[1]
    span = rows + HEADER
    for s in range(slabs):
        here = slice(s * span, (s + 1) * span)
        gate = convolved(gate_low[here], taps[0], rows)
        up = convolved(up_low[here], taps[1], rows)
        out[s] = (gate * jax.nn.sigmoid(gate) * up).astype(BF16)


def hidden_units(features, edges, gate_w, up_w, taps):
    slabs, rows, width = features.shape
    columns = gate_w.shape[1]
    tile = 256
    weight = pl.BlockSpec((width, tile), lambda i: (0, i))
    return pl.pallas_call(
        functools.partial(hidden_kernel, slabs),
        grid=(columns // tile,),
        in_specs=[
            pl.BlockSpec(features.shape, lambda i: (0, 0, 0)),
            pl.BlockSpec(edges.shape, lambda i: (0, 0, 0)),
            weight,
            weight,
            pl.BlockSpec((2, TAPS, tile), lambda i: (0, 0, i)),
        ],
        out_specs=pl.BlockSpec((slabs, rows, tile), lambda i: (0, 0, i)),
        out_shape=jax.ShapeDtypeStruct((slabs, rows, columns), BF16),
        compiler_params=kernel_params(dims=("arbitrary",)),
        name="hidden_units",
    )(features, edges, gate_w, up_w, taps)


def down_kernel(hidden, weights, out):
    slabs, rows, _ = hidden.shape
    for s in range(slabs):
        out[s] = mm(hidden[s], weights[...], ((1,), (1,))).astype(BF16)


def narrowed(hidden, weights):
    slabs, rows, columns = hidden.shape
    width = weights.shape[0]
    tile = 256
    return pl.pallas_call(
        down_kernel,
        grid=(width // tile,),
        in_specs=[
            pl.BlockSpec(hidden.shape, lambda i: (0, 0, 0)),
            pl.BlockSpec((tile, columns), lambda i: (i, 0)),
        ],
        out_specs=pl.BlockSpec((slabs, rows, tile), lambda i: (0, 0, i)),
        out_shape=jax.ShapeDtypeStruct((slabs, rows, width), BF16),
        compiler_params=kernel_params(dims=("arbitrary",)),
        name="narrowed",
    )(hidden, weights)


def exchanged(piece, axis):
    pieces = {0: piece}
    mask = lax.axis_size(axis) // 2
    while mask >= 1:
        for d in list(pieces):
            pieces[d ^ mask] = swapped(pieces[d], axis, mask)
        mask //= 2
    return [pieces[d] for d in sorted(pieces)]


def per_device(
    arriving_hidden_state,
    former_request_vectors,
    former_match_vectors,
    latter_request_vectors,
    latter_match_vectors,
    stored_vectors_both,
    closing_valve_operands,
    update_level_before_squash,
    fading_data_input,
    sparse_fading_boost,
    unitwise_fading_loglevel,
    fading_constant_term,
    unitwise_normalizer_coef,
    emission_map_weights,
    channel_normalizer_coef,
    switching_channel_map,
    broadening_channel_map,
    timewise_convolve_tapvalues,
    narrowing_map_weights_in,
):
    whole_gate, whole_up, whole_down = (
        lax.all_gather(w, "sp", axis=0, tiled=True)
        for w in (switching_channel_map, broadening_channel_map, narrowing_map_weights_in)
    )
    rows, groups, _ = stored_vectors_both.shape
    count = unitwise_fading_loglevel.shape[1]
    heads = groups * count
    value_size = stored_vectors_both.shape[2] // count
    head_sizes = tuple(
        (a.shape[1] // count, count) for a in (former_request_vectors, latter_request_vectors)
    )
    flat = lambda a: a.reshape(heads, -1)
    local, reach, summary = attention_pass(
        head_sizes,
        (former_request_vectors, latter_request_vectors),
        (former_match_vectors, latter_match_vectors),
        stored_vectors_both.reshape(rows, -1),
        flat(update_level_before_squash),
        flat(fading_data_input),
        flat(sparse_fading_boost),
        flat(unitwise_fading_loglevel),
        flat(fading_constant_term),
    )
    odd, before, partner = state_before(head_sizes, value_size, summary)
    attended = finish_heads(
        head_sizes,
        value_size,
        odd,
        before,
        partner,
        local,
        reach,
        closing_valve_operands.reshape(rows, -1),
        unitwise_normalizer_coef[None, :],
    )
    split = lax.axis_size("tp")
    arrived = lax.all_to_all(attended.reshape(split, rows // split, -1), "tp", 0, 0, tiled=False)
    resid, normed = emission(
        arrived,
        emission_map_weights,
        arriving_hidden_state,
        channel_normalizer_coef[None, :],
        groups,
    )
    edge = shifted(normed[-HEADER:], ("sp", "tp"), 1)
    features = jnp.stack(exchanged(normed, "tp"))
    edges = jnp.stack(exchanged(edge, "tp"))
    taps = timewise_convolve_tapvalues.astype(F32).transpose(1, 0, 2)
    hidden = hidden_units(features, edges, whole_gate, whole_up, taps)
    partial = narrowed(hidden, whole_down)
    pieces = [partial[d] for d in range(split)]
    mask = 1
    while mask < split:
        kept = [d for d in range(0, split, 2 * mask)]
        pieces_next = {}
        for d in kept:
            got = swapped(pieces[d ^ mask], "tp", mask)
            pieces_next[d] = (pieces[d].astype(F32) + got.astype(F32)).astype(BF16)
        pieces = {d: pieces_next[d] for d in kept}
        mask *= 2
    return (resid + pieces[0].astype(F32)).astype(BF16)


def solution(mesh):
    placed = (
        P(("sp", "tp"), None),
        P("sp", "tp"),
        P("sp", "tp"),
        P("sp", "tp"),
        P("sp", "tp"),
        P("sp", None, "tp"),
        P("sp", None, "tp"),
        P(None, "tp", "sp"),
        P(None, "tp", "sp"),
        P(None, "tp", "sp"),
        P(None, "tp"),
        P(None, "tp"),
        P(),
        P(),
        P(),
        P("sp", "tp"),
        P("sp", "tp"),
        P(None, None, "tp"),
        P("sp", "tp"),
    )
    return jax.shard_map(
        per_device, mesh=mesh, in_specs=placed, out_specs=P(("sp", "tp"), None), check_vma=False
    )
```

```python
import functools

import jax
import jax.numpy as jnp
from jax import lax
from jax.experimental import pallas as pl
from jax.experimental.pallas import tpu as pltpu
from jax.sharding import PartitionSpec as P


TAPS = 3
EPSILON = 1e-06
PRECISE = lax.Precision.HIGHEST
CHUNK = 128
HEADER = 8
CHUNKS = 2
F32 = jnp.float32
BF16 = jnp.bfloat16


def mm(a, b, dims=((1,), (0,))):
    return lax.dot_general(a, b, (dims, ((), ())), preferred_element_type=F32)


def exact(a, b, dims=((1,), (0,))):
    return lax.dot_general(a, b, (dims, ((), ())), precision=PRECISE, preferred_element_type=F32)


def kernel_params(mebibytes=56, dims=None):
    return pltpu.CompilerParams(vmem_limit_bytes=mebibytes << 20, dimension_semantics=dims)


def chunk_kernel(head_sizes, value_size, step_chunks, *refs):
    (update, data, spike, level, bias, *rest) = refs
    groups = len(head_sizes)
    queries = rest[:groups]
    keys = rest[groups : 2 * groups]
    values, out_local, out_reach, state_out, state = rest[2 * groups :]
    heads = []
    top = 0
    for g, (key_size, count) in enumerate(head_sizes):
        for h in range(count):
            heads.append((g, h * key_size, key_size, top))
            top += key_size

    @pl.when(pl.program_id(0) == 0)
    def _():
        for _g, _c, key_size, start in heads:
            rows = lax.broadcasted_iota(jnp.int32, (key_size, 2 * value_size), 0)
            cols = lax.broadcasted_iota(jnp.int32, (key_size, 2 * value_size), 1)
            state[pl.ds(start, key_size), :] = (cols == rows + value_size).astype(F32)

    size = CHUNK
    row = lax.broadcasted_iota(jnp.int32, (size, size), 0)
    col = lax.broadcasted_iota(jnp.int32, (size, size), 1)
    apart = row ^ col
    causal = row >= col
    triangle = causal.astype(F32)
    unit = (row == col).astype(F32)
    stacked = lambda ref: jnp.concatenate([ref[g] for g in range(groups)], axis=0)
    beta_all = jax.nn.sigmoid(stacked(update).astype(F32))
    biased = stacked(data) + bias[...]
    softplus = jnp.maximum(biased, 0.0) + jnp.log(1.0 + jnp.exp(-jnp.abs(biased)))
    gates_all = -jnp.exp(level[...]) * softplus + stacked(spike)

    units = [(sub, n) for sub in range(step_chunks) for n in range(len(heads))]
    cum_row, cum_col, beta_col, grown = {}, {}, {}, {}
    for sub in range(step_chunks):
        lo = sub * size
        gates = gates_all[:, lo : lo + size]
        cum_row[sub] = exact(gates, triangle, ((1,), (1,)))
        cum_col[sub] = exact(triangle, gates, ((1,), (1,)))
        beta_col[sub] = exact(unit, beta_all[:, lo : lo + size], ((1,), (1,)))
        grown[sub] = jnp.exp(cum_col[sub])

    def unit_rows(ref, lo, at, key_size, scale):
        full = ref[pl.ds(lo, size), at : at + key_size].astype(F32)
        size_of = lax.rsqrt(jnp.sum(full * full, axis=1, keepdims=True) + EPSILON)
        return full * (size_of * scale)

    kf, kb, lower, intra, right, qd = {}, {}, {}, {}, {}, {}
    for u in units:
        sub, n = u
        g, at, key_size, _ = heads[n]
        lo = sub * size
        kf[u] = unit_rows(keys[g], lo, at, key_size, 1.0)
        kb[u] = kf[u].astype(BF16)
        qf = unit_rows(queries[g], lo, at, key_size, key_size**-0.5)
        both = mm(jnp.concatenate([kb[u], qf.astype(BF16)], axis=0), kb[u], ((1,), (1,)))
        cum = cum_col[sub][:, n : n + 1]
        beta = beta_col[sub][:, n : n + 1]
        grow = grown[sub][:, n : n + 1]
        decay = jnp.exp(jnp.where(causal, cum - cum_row[sub][n : n + 1], -1e30))
        lower[u] = both[:size] * decay * beta
        intra[u] = (both[size:] * decay).astype(BF16)
        vf = values[pl.ds(lo, size), n * value_size : (n + 1) * value_size].astype(F32)
        right[u] = jnp.concatenate([vf * beta, kf[u] * (beta * grow)], axis=1).astype(BF16)
        qd[u] = (qf * grow).astype(BF16)
    inverse = {}
    for u in units:
        inverse[u] = unit - jnp.where((apart == 1) & causal, lower[u], 0.0)
    width = 2
    while width < size:
        here = (apart >= width) & (apart < 2 * width) & causal
        xb, inner = {}, {}
        for u in units:
            xb[u] = inverse[u].astype(BF16)
            inner[u] = mm(jnp.where(here, lower[u], 0.0).astype(BF16), xb[u]).astype(BF16)
        for u in units:
            inverse[u] = inverse[u] - mm(xb[u], inner[u])
        width *= 2
    solved = {}
    for u in units:
        solved[u] = mm(inverse[u].astype(BF16), right[u])

    for sub in range(step_chunks):
        lo = sub * size
        old, old_b, fresh, result = {}, {}, {}, {}
        for n, (_g, _at, key_size, start) in enumerate(heads):
            old[n] = state[pl.ds(start, key_size), :]
            old_b[n] = old[n].astype(BF16)
        for n in range(len(heads)):
            both = solved[(sub, n)]
            pulled = mm(both[:, value_size:].astype(BF16), old_b[n])
            fresh[n] = jnp.concatenate(
                [both[:, :value_size] - pulled[:, :value_size], -pulled[:, value_size:]], axis=1
            )
        for n, (_g, _at, key_size, start) in enumerate(heads):
            u = (sub, n)
            last = cum_row[sub][n : n + 1, size - 1 : size]
            fade = jnp.exp(last - cum_col[sub][:, n : n + 1])
            kept = (kf[u] * fade).astype(BF16)
            fb = fresh[n].astype(BF16)
            state[pl.ds(start, key_size), :] = old[n] * jnp.exp(last) + mm(kept, fb, ((0,), (0,)))
            result[n] = mm(
                jnp.concatenate([intra[u], qd[u]], axis=1), jnp.concatenate([fb, old_b[n]], axis=0)
            )
            out_local[pl.ds(lo, size), n * value_size : (n + 1) * value_size] = result[n][
                :, :value_size
            ]
        left = 0
        for g, (key_size, count) in enumerate(head_sizes):
            reach = jnp.concatenate(
                [
                    result[n][:, value_size : value_size + key_size]
                    for n, head in enumerate(heads)
                    if head[0] == g
                ],
                axis=1,
            )
            out_reach[pl.ds(lo, size), left : left + reach.shape[1]] = reach.astype(BF16)
            left += reach.shape[1]

    @pl.when(pl.program_id(0) == pl.num_programs(0) - 1)
    def _():
        state_out[...] = state[...].astype(BF16)


def attention_pass(head_sizes, queries, keys, values, update, data, spike, level, bias):
    rows = values.shape[0]
    heads = sum(c for _, c in head_sizes)
    value_size = values.shape[1] // heads
    step_chunks = 2
    tile = CHUNK * step_chunks
    key_cols = sum(k * c for k, c in head_sizes)
    by_rows = lambda a: pl.BlockSpec((tile, a.shape[1]), lambda i: (i, 0))
    by_cols = lambda a: pl.BlockSpec((*a.shape[:2], tile), lambda i: (0, 0, i))
    whole = lambda a: pl.BlockSpec(a.shape, lambda i: (0, 0))
    return pl.pallas_call(
        functools.partial(chunk_kernel, head_sizes, value_size, step_chunks),
        grid=(rows // tile,),
        in_specs=[by_cols(update), by_cols(data), by_cols(spike), whole(level), whole(bias)]
        + [by_rows(a) for a in (*queries, *keys, values)],
        out_specs=[
            pl.BlockSpec((tile, heads * value_size), lambda i: (i, 0)),
            pl.BlockSpec((tile, key_cols), lambda i: (i, 0)),
            pl.BlockSpec((key_cols, 2 * value_size), lambda i: (0, 0)),
        ],
        out_shape=[
            jax.ShapeDtypeStruct((rows, heads * value_size), F32),
            jax.ShapeDtypeStruct((rows, key_cols), BF16),
            jax.ShapeDtypeStruct((key_cols, 2 * value_size), BF16),
        ],
        scratch_shapes=[pltpu.VMEM((key_cols, 2 * value_size), F32)],
        compiler_params=kernel_params(dims=("arbitrary",)),
        name="attention_pass",
    )(update, data, spike, level, bias, *queries, *keys, values)


def joined(head_sizes, value_size, later, earlier, columns):
    parts = []
    top = 0
    for key_size, count in head_sizes:
        for _ in range(count):
            moves = later[top : top + key_size, value_size : value_size + key_size]
            new = mm(moves, earlier[top : top + key_size, :columns])
            adds = later[top : top + key_size, :value_size].astype(F32)
            if columns > value_size:
                new = jnp.concatenate([new[:, :value_size] + adds, new[:, value_size:]], axis=1)
            else:
                new = new + adds
            parts.append(new)
            top += key_size
    return jnp.concatenate(parts, axis=0)


def pair_kernel(head_sizes, value_size, odd, own, other, out):
    is_odd = odd[0] == 1
    mine = own[...]
    theirs = other[...]
    later = jnp.where(is_odd, mine, theirs)
    earlier = jnp.where(is_odd, theirs, mine)
    out[...] = joined(head_sizes, value_size, later, earlier, mine.shape[1]).astype(BF16)


def chain_kernel(head_sizes, value_size, later, earlier, out):
    out[...] = joined(head_sizes, value_size, later[...], earlier[...], out.shape[1]).astype(BF16)


def join_pair(head_sizes, value_size, odd, own, other):
    return pl.pallas_call(
        functools.partial(pair_kernel, head_sizes, value_size),
        in_specs=[pl.BlockSpec(memory_space=pltpu.SMEM), pl.BlockSpec(), pl.BlockSpec()],
        out_shape=jax.ShapeDtypeStruct(own.shape, BF16),
        name="join_pair",
    )(odd, own, other)


def join_chain(head_sizes, value_size, later, earlier):
    return pl.pallas_call(
        functools.partial(chain_kernel, head_sizes, value_size),
        out_shape=jax.ShapeDtypeStruct(earlier.shape, BF16),
        name="join_chain",
    )(later, earlier)


def shifted(value, axis, steps):
    count = lax.axis_size(axis)
    return lax.ppermute(value, axis, [(i, i + steps) for i in range(count - steps)])


def swapped(value, axis, mask):
    count = lax.axis_size(axis)
    return lax.ppermute(value, axis, [(i, i ^ mask) for i in range(count)])


def state_before(head_sizes, value_size, summary):
    count = lax.axis_size("sp")
    odd = jnp.full((1,), lax.axis_index("sp") % 2, jnp.int32)
    partner = swapped(summary, "sp", 1)
    pair = join_pair(head_sizes, value_size, odd, summary, partner)
    before = shifted(pair, "sp", 2)
    covered, pairs = 1, count // 2
    while covered < pairs - 1:
        window = join_chain(head_sizes, value_size, pair, before)
        reach = covered + 1
        finishing = covered + reach >= pairs - 1
        sent = window[:, :value_size] if finishing else window
        arrived = shifted(sent, "sp", 2 * reach)
        before = join_chain(head_sizes, value_size, before, arrived)
        covered += reach
    return before[:, :value_size], partner


def finish_kernel(head_sizes, value_size, place, before, partner, local, reach, gates, coef, out, initial):
    @pl.when(pl.program_id(0) == 0)
    def _():
        entering = before[...]
        through = joined(head_sizes, value_size, partner[...], entering, value_size)
        initial[...] = jnp.where(place[0] == 1, through, entering.astype(F32)).astype(BF16)

    top = 0
    number = 0
    for key_size, count in head_sizes:
        for _ in range(count):
            cols = slice(number * value_size, (number + 1) * value_size)
            full = local[:, cols] + mm(
                reach[:, top : top + key_size], initial[pl.ds(top, key_size), :]
            )
            gate = gates[:, cols].astype(F32)
            size = lax.rsqrt(jnp.mean(full * full, axis=1, keepdims=True) + EPSILON)
            out[0, :, cols] = (full * size * coef[...] * (gate * jax.nn.sigmoid(gate))).astype(BF16)
            top += key_size
            number += 1


def finish_heads(head_sizes, value_size, place, before, partner, local, reach, gates, coef, split):
    rows, width = local.shape
    tile = rows // split
    by_rows = lambda a: pl.BlockSpec((tile, a.shape[1]), lambda i, place: (i, 0))
    whole = lambda a: pl.BlockSpec(a.shape, lambda i, place: (0, 0))
    return pl.pallas_call(
        functools.partial(finish_kernel, head_sizes, value_size),
        grid_spec=pltpu.PrefetchScalarGridSpec(
            num_scalar_prefetch=1,
            grid=(split,),
            in_specs=[
                whole(before),
                whole(partner),
                by_rows(local),
                by_rows(reach),
                by_rows(gates),
                whole(coef),
            ],
            out_specs=pl.BlockSpec((1, tile, width), lambda i, place: (i ^ place[1], 0, 0)),
            scratch_shapes=[pltpu.VMEM(before.shape, BF16)],
        ),
        out_shape=jax.ShapeDtypeStruct((split, tile, width), BF16),
        compiler_params=kernel_params(dims=("arbitrary",)),
        name="finish_heads",
    )(place, before, partner, local, reach, gates, coef)


def emission_kernel(groups, place, *refs):
    split = len(refs) - 7
    pieces = refs[:split]
    weights, stream, coef, resid, normed, last, tail = refs[split:]
    part = pieces[0].shape[1] // groups
    full = stream[...].astype(F32)
    for d in range(split):
        for g in range(groups):
            top = pl.multiple_of((g * split + (place[1] ^ d)) * part, part)
            full += mm(pieces[d][:, g * part : (g + 1) * part], weights[pl.ds(top, part), :])
    resid[...] = full
    size = lax.rsqrt(jnp.mean(full * full, axis=1, keepdims=True) + EPSILON)
    done = (full * size * coef[...]).astype(BF16)
    normed[...] = done
    last[...] = done[done.shape[0] - last.shape[0] :]
    tail[...] = done[done.shape[0] - HEADER :]


def emission(place, pieces, weights, stream, coef, groups):
    rows, width = stream.shape
    vmem = pl.BlockSpec(memory_space=pltpu.VMEM)
    return pl.pallas_call(
        functools.partial(emission_kernel, groups),
        in_specs=[pl.BlockSpec(memory_space=pltpu.SMEM)] + [vmem] * (len(pieces) + 3),
        out_specs=[vmem] * 4,
        out_shape=[
            jax.ShapeDtypeStruct((rows, width), F32),
            jax.ShapeDtypeStruct((rows, width), BF16),
            jax.ShapeDtypeStruct((rows // CHUNKS + HEADER, width), BF16),
            jax.ShapeDtypeStruct((HEADER, width), BF16),
        ],
        compiler_params=kernel_params(24),
        name="emission",
    )(place, *pieces, weights, stream, coef)


def convolved(low, taps, rows):
    total = None
    for j in range(TAPS):
        start = HEADER - (TAPS - 1) + j
        term = taps[j : j + 1, :] * low[start : start + rows, :]
        total = term if total is None else total + term
    return total


def hidden_kernel(slabs, blocks, place, *refs):
    features = refs[:slabs]
    gate_w = refs[slabs : slabs + blocks]
    up_w = refs[slabs + blocks : slabs + 2 * blocks]
    taps, out, taken = refs[slabs + 2 * blocks :]
    span = features[0].shape[0]
    rows = span - HEADER

    @pl.when(pl.program_id(0) == 0)
    def _():
        block = features[0].shape[1] // blocks
        for e in range(blocks):
            source = pl.multiple_of((place[2] ^ e) * block, block)
            for s in range(slabs):
                taken[pl.ds(s * span, span), e * block : (e + 1) * block] = features[s][
                    :, pl.ds(source, block)
                ]

    def low(pieces):
        weights = jnp.concatenate([piece[...] for piece in pieces], axis=0)
        return mm(taken[...], weights).astype(BF16).astype(F32)

    gate_low = low(gate_w)
    up_low = low(up_w)
    for s in range(slabs):
        here = slice(s * span, (s + 1) * span)
        gate = convolved(gate_low[here], taps[0], rows)
        up = convolved(up_low[here], taps[1], rows)
        out[pl.ds(s * rows, rows), :] = (gate * jax.nn.sigmoid(gate) * up).astype(BF16)


def hidden_units(place, features, both_w, taps):
    span, width = features[0].shape
    slabs, blocks = len(features), len(both_w)
    block, columns = both_w[0].shape
    columns //= 2
    tile = 256 if columns % 256 == 0 else 128
    shift = columns // tile
    whole = pl.BlockSpec((span, width), lambda i, place: (0, 0))
    return pl.pallas_call(
        functools.partial(hidden_kernel, slabs, blocks),
        grid_spec=pltpu.PrefetchScalarGridSpec(
            num_scalar_prefetch=1,
            grid=(shift,),
            in_specs=[whole] * slabs
            + [pl.BlockSpec((block, tile), lambda i, place: (0, i))] * blocks
            + [pl.BlockSpec((block, tile), lambda i, place: (0, i + shift))] * blocks
            + [pl.BlockSpec((2, TAPS, tile), lambda i, place: (0, 0, i))],
            out_specs=pl.BlockSpec((slabs * (span - HEADER), tile), lambda i, place: (0, i)),
            scratch_shapes=[pltpu.VMEM((slabs * span, width), BF16)],
        ),
        out_shape=jax.ShapeDtypeStruct((slabs * (span - HEADER), columns), BF16),
        compiler_params=kernel_params(32, ("arbitrary",)),
        name="hidden_units",
    )(place, *features, *both_w, *both_w, taps)


def down_kernel(split, place, hidden, *refs):
    weights, keep, send = refs[:-2], refs[-2], refs[-1]
    rows = hidden.shape[0] // split
    tile = weights[0].shape[0]
    for e, piece in enumerate(weights):
        part = mm(hidden[...], piece[...], ((1,), (1,)))
        spot = pl.ds(pl.multiple_of((place[2] ^ e) * tile, tile), tile)
        for d in range(split):
            here = part[d * rows : (d + 1) * rows]
            if d % 2 == 0:
                keep[d // 2, :, spot] = here
            else:
                send[d // 2, :, spot] = here.astype(BF16)


def narrowed(place, hidden, weights, split):
    rows, _ = hidden.shape
    width = weights[0].shape[0] * len(weights)
    vmem = pl.BlockSpec(memory_space=pltpu.VMEM)
    shape = (split // 2, rows // split, width)
    return pl.pallas_call(
        functools.partial(down_kernel, split),
        in_specs=[pl.BlockSpec(memory_space=pltpu.SMEM)] + [vmem] * (len(weights) + 1),
        out_specs=[vmem, vmem],
        out_shape=[jax.ShapeDtypeStruct(shape, F32), jax.ShapeDtypeStruct(shape, BF16)],
        compiler_params=kernel_params(24),
        name="narrowed",
    )(place, hidden, *weights)


def exchanged(piece, axis):
    pieces = {0: piece}
    mask = lax.axis_size(axis) // 2
    while mask >= 1:
        for d in list(pieces):
            pieces[d ^ mask] = swapped(pieces[d], axis, mask)
        mask //= 2
    return [pieces[d] for d in sorted(pieces)]


def summed(keep, send, axis):
    got = swapped(send, axis, 1)
    total = keep + got.astype(F32)
    mask = 2
    while mask < lax.axis_size(axis):
        kept, sent = total[0::2], total[1::2]
        got = swapped(sent.astype(BF16), axis, mask)
        total = kept + got.astype(F32)
        mask *= 2
    return total[0]


def per_device(
    arriving_hidden_state,
    former_request_vectors,
    former_match_vectors,
    latter_request_vectors,
    latter_match_vectors,
    stored_vectors_both,
    closing_valve_operands,
    update_level_before_squash,
    fading_data_input,
    sparse_fading_boost,
    unitwise_fading_loglevel,
    fading_constant_term,
    unitwise_normalizer_coef,
    emission_map_weights,
    channel_normalizer_coef,
    switching_channel_map,
    broadening_channel_map,
    timewise_convolve_tapvalues,
    narrowing_map_weights_in,
):
    rows, groups, _ = stored_vectors_both.shape
    count = unitwise_fading_loglevel.shape[1]
    heads = groups * count
    value_size = stored_vectors_both.shape[2] // count
    split = lax.axis_size("tp")
    ring = lax.axis_size("sp")
    half = ring // 2
    at_sp = lax.axis_index("sp")
    at_tp = lax.axis_index("tp")
    upper = at_sp // half
    place = jnp.stack([at_sp % 2, at_tp, at_sp]).astype(jnp.int32)
    across = half

    columns = switching_channel_map.shape[1] // 2

    def mine(w, which):
        return lax.dynamic_slice_in_dim(w, which * columns, columns, 1)

    def halves(ws):
        return [jnp.concatenate([mine(w, w_at) for w in ws], axis=1) for w_at in (upper, 1 - upper)]

    def spread(piece, masks, tie=lambda a: a):
        pieces = {0: piece}
        for mask in masks:
            for d in list(pieces):
                source = tie(pieces[d]) if d else pieces[d]
                pieces[d ^ mask] = swapped(source, "sp", mask)
        return pieces

    masks = [1 << bit for bit in range(half.bit_length() - 1)]
    both_kept, both_sent = halves((switching_channel_map, broadening_channel_map))
    down_kept, down_sent = halves((narrowing_map_weights_in,))
    both_got = swapped(both_sent, "sp", across)

    head_sizes = tuple(
        (a.shape[1] // count, count) for a in (former_request_vectors, latter_request_vectors)
    )
    local, reach, summary = attention_pass(
        head_sizes,
        (former_request_vectors, latter_request_vectors),
        (former_match_vectors, latter_match_vectors),
        stored_vectors_both.reshape(rows, -1),
        update_level_before_squash,
        fading_data_input,
        sparse_fading_boost,
        unitwise_fading_loglevel.reshape(heads, 1),
        fading_constant_term.reshape(heads, 1),
    )
    before, partner = state_before(head_sizes, value_size, summary)
    tie = lambda a: lax.optimization_barrier((a, before))[0]
    down_got = swapped(tie(down_sent), "sp", across)

    def all_pieces(kept, got):
        pieces = spread(kept, masks, tie)
        pieces.update({d ^ half: a for d, a in spread(got, masks[::-1]).items()})
        return [pieces[e] for e in range(ring)]

    both_w = all_pieces(both_kept, both_got)
    down_w = all_pieces(down_kept, down_got)
    attended = finish_heads(
        head_sizes,
        value_size,
        place,
        before,
        partner,
        local,
        reach,
        closing_valve_operands.reshape(rows, -1),
        unitwise_normalizer_coef[None, :],
        split,
    )
    pieces = [attended[0]] + [swapped(attended[d], "tp", d) for d in range(1, split)]
    resid, normed, last, tail = emission(
        place,
        pieces,
        emission_map_weights,
        arriving_hidden_state,
        channel_normalizer_coef[None, :],
        groups,
    )
    edge = shifted(tail, ("sp", "tp"), 1)
    slab = jnp.concatenate([edge, normed], axis=0)
    first = slab[: last.shape[0]]
    far_last = swapped(last, "sp", across)
    far_first = swapped(first, "sp", across)

    taps = mine(timewise_convolve_tapvalues.astype(F32).transpose(1, 0, 2).reshape(2 * TAPS, -1), upper)
    taps = taps.reshape(2, TAPS, -1)

    def sums(features):
        hidden = hidden_units(place, features, both_w, taps)
        return summed(*narrowed(place, hidden, down_w, split), "tp")

    near = sums(exchanged(slab, "tp"))
    outs = []
    for number, far in ((1, far_last), (0, far_first)):
        total = sums(exchanged(far, "tp"))
        outs.append((number, swapped(total.astype(BF16), "sp", across)))
    outs = jnp.concatenate([got for _n, got in sorted(outs, key=lambda pair: pair[0])], axis=0)
    return (resid + near + outs.astype(F32)).astype(BF16)


def solution(mesh):
    placed = (
        P(("sp", "tp"), None),
        P("sp", "tp"),
        P("sp", "tp"),
        P("sp", "tp"),
        P("sp", "tp"),
        P("sp", None, "tp"),
        P("sp", None, "tp"),
        P(None, "tp", "sp"),
        P(None, "tp", "sp"),
        P(None, "tp", "sp"),
        P(None, "tp"),
        P(None, "tp"),
        P(),
        P(),
        P(),
        P("sp", "tp"),
        P("sp", "tp"),
        P(None, None, "tp"),
        P("sp", "tp"),
    )

    return jax.shard_map(
        per_device, mesh=mesh, in_specs=placed, out_specs=P(("sp", "tp"), None), check_vma=False
    )
```
